32 devices in a mesh: row: 8 (over z, x), col: 4 (over y, core).
Axes of the slice: x: 2, y: 2, z: 4, core: 2. Of those that a mesh axis runs over, the one named last changes fastest.
Arguments:
- tokens: bfloat16 [8192, 2048], P('row'), may hold values from -136 to 136
- norm_gain: float32 [2048], replicated, may hold values from 0.1 to 1.9
- w_in: bfloat16 [2048, 1024], P(None, 'col'), may hold values from -0.125 to 0.125
- w_out: bfloat16 [1024, 2048], P(None, 'col'), may hold values from -0.1875 to 0.1875
Outputs:
- mixed_tokens: bfloat16 [8192, 2048], P('row', 'col')
The draws below stay inside these ranges and needn't reach their ends.
All inputs are finite; a program needn't handle non-finite values.
Results may differ from the reference program's by a relative error of at most 0.013.
Values may be sent and summed in bfloat16 or wider, within the bound.
A program may use at most 64 MiB of HBM per device.

```python
import math
import jax
import jax.numpy as jnp
from jax import lax

D = 2048
FW = 1024
GROUP = 256
GROUPS = 4
LENGTH = 8192


def draw_tokens(key, part):
    key_values, key_scales = jax.random.split(key, 2)
    columns = jnp.arange(D, dtype=jnp.float32) / D
    values = jnp.clip(jax.random.normal(key_values, (LENGTH, D), jnp.float32), -6.0, 6.0)
    row_scale = jnp.exp(jax.random.uniform(key_scales, (LENGTH, 1), jnp.float32, 0.0, 0.2))
    col_scale = jnp.exp(columns * math.log(4.0))
    return (values * row_scale * col_scale[None, :]).astype(jnp.bfloat16)


def level_of(own_key, extent, cuts, smallest, high):
    factor_of, own = 1.0, jax.random.fold_in(own_key, 6)
    for position, shards_of in cuts:
        steps = jnp.exp(jax.random.uniform(jax.random.fold_in(own, position), (shards_of,), jnp.float32, smallest / len(cuts), high / len(cuts)))
        factor_of = factor_of * jnp.repeat(steps, extent[position] // shards_of).reshape([-1 if axis == position else 1 for axis in range(len(extent))])
    return factor_of


def bell_draw(rng, dims, spread, most, cuts=(), kind=jnp.bfloat16):
    drawn = jax.random.normal(rng, dims, jnp.float32) * spread
    if len(cuts) > 0:
        drawn = level_of(rng, dims, cuts, -0.22, 0.18) * drawn
    return jnp.clip(drawn, min=-most, max=most).astype(kind)


def setup_inputs(seed: int = 0) -> dict:
    keys = jax.random.split(jax.random.key(seed), 5)
    tokens = draw_tokens(jax.random.fold_in(keys[4], 71), 0)
    norm_gain = jnp.clip(1.0 + 0.18 * jax.random.normal(keys[1], (D,), jnp.float32), 0.1, 1.9)
    w_in = bell_draw(keys[2], (D, FW), D ** -0.5, 0.125, ((1, 4),))
    w_out = bell_draw(keys[3], (FW, D), FW ** -0.5, 0.1875, ((1, 4),))
    return {"tokens": tokens, "norm_gain": norm_gain, "w_in": w_in, "w_out": w_out}


NORM_EPS = 1e-06

def reference(tokens, norm_gain, w_in, w_out):
    widened = tokens.astype(jnp.float32)
    inverse = lax.rsqrt(lax.optimization_barrier(jnp.mean(widened * widened, axis=1, keepdims=True)) + NORM_EPS)
    normed = (widened * inverse * norm_gain[None, :]).astype(jnp.bfloat16)
    projected = jnp.dot(normed, w_in, preferred_element_type=jnp.float32).astype(jnp.bfloat16)
    grouped = projected.astype(jnp.float32).reshape(LENGTH, GROUPS, GROUP)
    spectrum = jnp.real(jnp.fft.fftn(grouped, axes=(0, 2), norm='ortho'))
    spectral = spectrum.reshape(LENGTH, FW).astype(jnp.bfloat16)
    return jnp.dot(spectral, w_out, preferred_element_type=jnp.float32).astype(jnp.bfloat16)
```

```python
import functools
import math

import jax
import jax.numpy as jnp
import numpy as np
from jax import lax
from jax.experimental import pallas as pl
from jax.experimental.pallas import tpu as pltpu
from jax.sharding import PartitionSpec as P

GROUP = 256


NORM_EPS = 1e-06


def as_sent(array):

    def short(part):
        return part.astype(jnp.bfloat16) if part.dtype == jnp.float32 else part

    return jax.tree.map(short, array)


def rotation_table(first_index, second_index, spectral_magnitude, factor):
    phase = (first_index * second_index % spectral_magnitude).astype(jnp.float32) * (
        2.0 * math.pi / spectral_magnitude
    )
    return (jnp.cos(phase) * factor, jnp.sin(phase) * factor)


def twiddle(real_input_values, imag_in, freq_index, pos_index, spectral_magnitude):
    cosine, sine = rotation_table(freq_index, pos_index, spectral_magnitude, 1.0)
    return (
        real_input_values * cosine + imag_in * sine,
        imag_in * cosine - real_input_values * sine,
    )


def second_section(stacked, half):
    length_dev = stacked.shape[1]
    stride = min(length_dev, 512)
    positions = lax.broadcasted_iota(jnp.int32, (length_dev, stride), 0)
    real_blocks = []
    imag_blocks = []
    for offset in range(0, length_dev, stride):
        freqs = lax.broadcasted_iota(jnp.int32, (length_dev, stride), 1) + offset
        cosine, sine = rotation_table(positions, freqs, length_dev, 1.0)
        with_cos = jnp.dot(stacked, cosine, precision=lax.Precision.HIGH)
        with_sin = jnp.dot(stacked, sine, precision=lax.Precision.HIGH)
        real_blocks.append(with_cos[:half] + with_sin[half:])
        imag_blocks.append(with_cos[half:] - with_sin[:half])
    return (jnp.concatenate(real_blocks, 1), jnp.concatenate(imag_blocks, 1))


def reorder_positions(arrived):
    channels, row_count, _, block_len = arrived.shape
    return jnp.swapaxes(arrived.reshape(channels, row_count, block_len), 1, 2).reshape(
        channels, row_count * block_len
    )


def local(tokens, norm_gain, w_in, w_out):
    length_dev = tokens.shape[0]
    row_count = lax.axis_size("row")
    col_count = lax.axis_size("col")
    total_len = length_dev * row_count
    widened = tokens.astype(jnp.float32)
    inverse = lax.rsqrt(jnp.mean(widened * widened, axis=1, keepdims=True) + NORM_EPS)
    normed = (widened * inverse * norm_gain[None, :]).astype(jnp.bfloat16)
    projected = lax.dot_general(
        w_in, normed, (((0,), (1,)), ((), ())), preferred_element_type=jnp.float32
    ).astype(jnp.bfloat16)
    channels = projected.shape[0]
    block_len = length_dev // row_count
    small_cos, small_sin = rotation_table(
        lax.broadcasted_iota(jnp.int32, (row_count, row_count), 0),
        lax.broadcasted_iota(jnp.int32, (row_count, row_count), 1),
        row_count,
        1.0 / math.sqrt(total_len),
    )
    per_row = channels // row_count
    arrived = lax.all_to_all(
        projected.reshape(channels, 1, length_dev), "row", split_axis=0, concat_axis=1, tiled=True
    )
    values = arrived.astype(jnp.float32)
    real_one = jnp.einsum("ka,cab->ckb", small_cos, values, precision=lax.Precision.HIGH)
    imag_one = -jnp.einsum("ka,cab->ckb", small_sin, values, precision=lax.Precision.HIGH)
    freq_index = lax.broadcasted_iota(jnp.int32, (row_count, length_dev), 0)
    pos_index = lax.broadcasted_iota(jnp.int32, (row_count, length_dev), 1)
    real_two, imag_two = twiddle(real_one, imag_one, freq_index, pos_index, total_len)
    stacked = jnp.concatenate(
        [
            real_two.reshape(per_row * row_count, length_dev),
            imag_two.reshape(per_row * row_count, length_dev),
        ],
        0,
    )
    real_three, imag_three = second_section(stacked, per_row * row_count)
    shaped = (per_row, row_count, row_count, block_len)
    back_real, back_imag = (
        lax.all_to_all(
            real_three.reshape(shaped).astype(jnp.bfloat16),
            "row",
            split_axis=2,
            concat_axis=0,
            tiled=True,
        ).astype(jnp.float32),
        lax.all_to_all(
            imag_three.reshape(shaped).astype(jnp.bfloat16),
            "row",
            split_axis=2,
            concat_axis=0,
            tiled=True,
        ).astype(jnp.float32),
    )
    spec_real = reorder_positions(back_real)
    spec_imag = reorder_positions(back_imag)
    quarter = length_dev // col_count
    group_cosine_table, group_sine_table = rotation_table(
        lax.broadcasted_iota(jnp.int32, (GROUP, GROUP), 0),
        lax.broadcasted_iota(jnp.int32, (GROUP, GROUP), 1),
        GROUP,
        1.0 / math.sqrt(GROUP),
    )
    real_input_values = lax.all_to_all(
        as_sent(spec_real.reshape(channels, col_count, quarter)),
        "col",
        split_axis=1,
        concat_axis=0,
        tiled=True,
    )
    imag_in = lax.all_to_all(
        as_sent(spec_imag.reshape(channels, col_count, quarter)),
        "col",
        split_axis=1,
        concat_axis=0,
        tiled=True,
    )
    width_all = real_input_values.shape[0]
    item_count = real_input_values.shape[2]
    groups = width_all // GROUP
    real_by_group = real_input_values.reshape(groups, GROUP, item_count)
    imaginary_by_group = imag_in.reshape(groups, GROUP, item_count)
    merged_spectrum = jnp.einsum(
        "hz,azo->aho", group_cosine_table, real_by_group, precision=lax.Precision.HIGH
    )
    merged_spectrum = merged_spectrum + jnp.einsum(
        "hz,azo->aho", group_sine_table, imaginary_by_group, precision=lax.Precision.HIGH
    )
    result = merged_spectrum.reshape(width_all, 1, item_count).astype(jnp.bfloat16)
    spectral = lax.all_to_all(result, "col", split_axis=0, concat_axis=1, tiled=True)
    output = lax.dot_general(
        lax.all_gather(spectral.reshape(channels, length_dev), "col", axis=0, tiled=True),
        w_out,
        (((0,), (0,)), ((), ())),
        preferred_element_type=jnp.float32,
    )
    return output.astype(jnp.bfloat16)


HALVES = 2
POINTS = 8
LANES = 128
MESH = pl.DeviceIdType.MESH


def channel_tables(group, total_len):
    half = group // 2
    index = np.arange(group)
    angle = 2.0 * np.pi * (index[:, None] * index[None, :] % group) / group
    transform = np.concatenate([np.cos(angle[: half + 1]), np.sin(angle[1:half])], 0)
    fold = np.zeros((group, group))
    for k in range(half + 1):
        fold[k, k] = 1.0
        fold[k, -k % group] = 1.0
    for k in range(1, half):
        fold[half + k, group - k] = 1.0
        fold[half + k, k] = -1.0
    return (transform / math.sqrt(group)).astype(jnp.bfloat16), fold.astype(jnp.bfloat16)


def position_tables(block, total_len):
    j = np.arange(block)
    angle = 2.0 * np.pi * (np.arange(POINTS)[:, None] * j[None, :]) / total_len
    twiddles = np.stack([np.cos(angle), np.sin(angle)]).astype(np.float32)
    root = 32
    coarse = 2.0 * np.pi * (np.arange(block // root)[:, None] * root * j[None, :] % block) / block
    fine = 2.0 * np.pi * (np.arange(root)[:, None] * j[None, :] % block) / block
    scale = 1.0 / math.sqrt(total_len)
    coarse = np.stack([np.cos(coarse), np.sin(coarse)]).astype(np.float32)
    fine = np.stack([np.cos(fine) * scale, np.sin(fine) * scale]).astype(np.float32)
    return twiddles, coarse, fine


def eight_points(x):
    a = [x[i] + x[i + 4] for i in range(4)]
    b = [x[i] - x[i + 4] for i in range(4)]
    even, odd = a[0] + a[2], a[1] + a[3]
    root = math.sqrt(0.5)
    minus, plus = root * (b[1] - b[3]), root * (b[1] + b[3])
    one = (b[0] + minus, -b[2] - plus)
    two = (a[0] - a[2], a[3] - a[1])
    three = (b[0] - minus, b[2] - plus)
    return [
        (even + odd, None),
        one,
        two,
        three,
        (even - odd, None),
        (three[0], -three[1]),
        (two[0], -two[1]),
        (one[0], -one[1]),
    ]


def mixer_kernel(
    steps,
    tokens_hbm, gain_hbm, w_in_hbm, w_out_hbm, forward_hbm, fold_hbm, twiddle_hbm, coarse_hbm, fine_hbm,
    out_ref,
    tokens, gain, w_in, w_out, forward, fold, twiddles, coarse, fine,
    packed, arrived, stage, table, ready, gathered, folded, total,
    token_sem, load_sem, own_sem, send_one, recv_one, send_two, recv_two, send_col, recv_col,
):
    row, col = lax.axis_index("row"), lax.axis_index("col")
    rows = packed.shape[1]
    block, width = packed.shape[3], w_in.shape[1]
    size = block // steps
    part = packed.shape[2]
    flip = lambda bit: col + bit - 2 * bit * (col // bit % 2)
    sibling, across = flip(1), flip(2)

    loads = [
        pltpu.make_async_copy(src, dst, load_sem.at[i])
        for i, (src, dst) in enumerate([
            (w_in_hbm, w_in), (gain_hbm, gain), (forward_hbm, forward), (coarse_hbm, coarse), (fine_hbm, fine),
            (twiddle_hbm, twiddles), (fold_hbm, fold), (w_out_hbm, w_out),
        ])
    ]
    token_loads = [
        pltpu.make_async_copy(
            tokens_hbm.at[pl.ds(p * size, size)], tokens.at[pl.ds(p * size, size)], token_sem.at[p]
        )
        for p in range(steps)
    ]
    for load in loads[:3]:
        load.start()
    for load in token_loads:
        load.start()
    for load in loads[3:]:
        load.start()

    barrier = pltpu.get_barrier_semaphore()
    peers = [(lax.rem(row + d, rows), col) for d in range(1, rows)] + [(row, sibling), (row, across)]
    for peer in peers:
        pl.semaphore_signal(barrier, inc=1, device_id=peer, device_id_type=MESH)

    def remote(src, dst, send, recv, device):
        return pltpu.make_async_remote_copy(
            src_ref=src, dst_ref=dst, send_sem=send, recv_sem=recv, device_id=device, device_id_type=MESH
        )

    def first_send(h, d, p=None):
        peer = lax.rem(row + d, rows)
        where = pl.ds(0, block) if p is None else pl.ds(p * size, size)
        return remote(
            packed.at[h, peer, :, where], arrived.at[h, row, :, where],
            send_one.at[h, d], recv_one.at[h, d], (peer, col),
        )

    order = [4, 3, 5, 2, 6, 1, 7]
    for load in loads[:3]:
        load.wait()
    for p in range(steps):
        token_loads[p].wait()
        where = slice(p * size, (p + 1) * size)
        wide = tokens[where, :].astype(jnp.float32)
        inverse = lax.rsqrt(jnp.mean(wide * wide, axis=1, keepdims=True) + NORM_EPS)
        normed = (wide * inverse * gain[...]).astype(jnp.bfloat16)
        projected = jnp.dot(normed, w_in[...], preferred_element_type=jnp.float32).astype(jnp.bfloat16)
        kept = lax.dot_general(
            forward[...], projected, (((1,), (1,)), ((), ())), preferred_element_type=jnp.float32
        )
        packed[:, :, :, where] = kept.astype(jnp.bfloat16).reshape(HALVES, rows, part, size)
        if p == 0:
            pl.semaphore_wait(barrier, len(peers))
        for d in order:
            first_send(0, d, p).start()
    for d in order:
        first_send(1, d).start()
    own_one = [
        pltpu.make_async_copy(packed.at[h, row], arrived.at[h, row], own_sem.at[h]) for h in range(HALVES)
    ]
    for copy in own_one:
        copy.start()
    for load in loads[3:]:
        load.wait()

    root = fine.shape[1]

    def table_rows(a, carry):
        cos_a, sin_a = coarse[0, pl.ds(a, 1), :], coarse[1, pl.ds(a, 1), :]
        at = pl.multiple_of(a * root, root)
        table[pl.ds(at, root), :] = (cos_a * fine[0] - sin_a * fine[1]).astype(jnp.bfloat16)
        table[pl.ds(block + at, root), :] = (sin_a * fine[0] + cos_a * fine[1]).astype(jnp.bfloat16)
        return carry

    lax.fori_loop(0, block // root, table_rows, 0)
    cols = w_out.shape[0] // width
    half = width // HALVES
    for c in range(cols):
        rows_out = jnp.dot(
            fold[...], w_out[c * width : (c + 1) * width, :], preferred_element_type=jnp.float32
        ).astype(jnp.bfloat16)
        for h in range(HALVES):
            folded[h, c * half : (c + 1) * half, :] = rows_out[h * half : (h + 1) * half]

    def second_send(h, d):
        peer = lax.rem(row + d, rows)
        return remote(
            ready.at[h, peer], gathered.at[h, col, row], send_two.at[h, d], recv_two.at[h, d], (peer, col)
        )

    own_two = [
        pltpu.make_async_copy(ready.at[h, row], gathered.at[h, col, row], own_sem.at[HALVES + h])
        for h in range(HALVES)
    ]
    for h in range(HALVES):
        own_one[h].wait()
        for d in order:
            first_send(h, d).wait_recv()

        def section(t, carry):
            at = pl.multiple_of(t * LANES, LANES)
            x = [arrived[h, r, :, pl.ds(at, LANES)].astype(jnp.float32) for r in range(rows)]
            points = eight_points(x)
            for k in range(POINTS):
                real, imag = points[k]
                if k > 0:
                    cosine = twiddles[0, k : k + 1, pl.ds(at, LANES)]
                    sine = twiddles[1, k : k + 1, pl.ds(at, LANES)]
                    if imag is None:
                        real, imag = real * cosine, -real * sine
                    else:
                        real, imag = real * cosine + imag * sine, imag * cosine - real * sine
                else:
                    imag = jnp.zeros_like(real)
                if h == 1:
                    place = lax.broadcasted_iota(jnp.int32, real.shape, 0) + row * part
                    plain = place == 0
                    real, imag = jnp.where(plain, real, -imag), jnp.where(plain, imag, real)
                stage[k, :, pl.ds(at, LANES)] = real.astype(jnp.bfloat16)
                stage[k, :, pl.ds(pl.multiple_of(block + at, LANES), LANES)] = imag.astype(jnp.bfloat16)
            return carry

        lax.fori_loop(0, block // LANES, section, 0)
        values = stage[...].reshape(POINTS * part, 2 * block)
        span = 2 * LANES
        for n in range(block // span):
            done = jnp.dot(
                values, table[:, n * span : (n + 1) * span], preferred_element_type=jnp.float32
            ).astype(jnp.bfloat16)
            for q in range(2):
                ready[h, 2 * n + q] = done[:, q * LANES : (q + 1) * LANES].reshape(POINTS, part, LANES)
        for d in order:
            second_send(h, d).start()
        own_two[h].start()

    def to_across(h, d, origin):
        spot = gathered.at[h, col, origin]
        return remote(spot, spot, send_col.at[h, 0, d], recv_col.at[h, 0, d], (row, across))

    def to_sibling(h, d, origin):
        spot = gathered.at[h, col, origin]
        return remote(spot, spot, send_col.at[h, 1, d], recv_col.at[h, 1, d], (row, sibling))

    def on_to_sibling(h, d, origin):
        spot = gathered.at[h, across, origin]
        return remote(spot, spot, send_col.at[h, 2, d], recv_col.at[h, 2, d], (row, sibling))

    near = [0, 1, 7, 2, 6, 3, 5, 4]
    origin_of = lambda d: lax.rem(row + rows - d, rows)
    for h in range(HALVES):
        for d in near:
            if d == 0:
                own_two[h].wait()
            else:
                second_send(h, d).wait_recv()
            to_across(h, d, origin_of(d)).start()
            to_sibling(h, d, origin_of(d)).start()
        for d in near:
            to_across(h, d, origin_of(d)).wait_recv()
            on_to_sibling(h, d, origin_of(d)).start()
        for d in near:
            to_sibling(h, d, origin_of(d)).wait_recv()
            on_to_sibling(h, d, origin_of(d)).wait_recv()
        for k in range(POINTS):
            spectrum = gathered[h, :, :, k].reshape(cols * rows * part, LANES)
            piece = lax.dot_general(
                spectrum, folded[h], (((0,), (0,)), ((), ())), preferred_element_type=jnp.float32
            )
            if h == 0:
                total[k] = piece
            else:
                scattered = total[k] + piece
                total[k] = scattered
    out_ref[...] = jnp.swapaxes(total[...], 0, 1).reshape(out_ref.shape).astype(out_ref.dtype)

    for h in range(HALVES):
        for d in order:
            first_send(h, d).wait_send()
            second_send(h, d).wait_send()
        for d in near:
            to_across(h, d, origin_of(d)).wait_send()
            to_sibling(h, d, origin_of(d)).wait_send()
            on_to_sibling(h, d, origin_of(d)).wait_send()


def fused(tokens, norm_gain, w_in, w_out):
    rows, cols = lax.axis_size("row"), lax.axis_size("col")
    block, width_in = tokens.shape
    width = w_in.shape[1]
    features = w_out.shape[1]
    part = width // (HALVES * rows)
    steps = 4
    forward, fold = channel_tables(width, block * rows)
    twiddles, coarse, fine = position_tables(block, block * rows)
    half, short, wide = jnp.bfloat16, pltpu.VMEM, jnp.float32
    operands = [tokens, norm_gain[None, :], w_in, w_out, forward, fold, twiddles, coarse, fine]
    operands = [jnp.asarray(x) for x in operands]
    dma = pltpu.SemaphoreType.DMA
    return pl.pallas_call(
        functools.partial(mixer_kernel, steps),
        out_shape=jax.ShapeDtypeStruct((block, features), half),
        in_specs=[pl.BlockSpec(memory_space=pl.ANY)] * len(operands),
        out_specs=pl.BlockSpec(memory_space=pltpu.VMEM),
        scratch_shapes=[short(x.shape, x.dtype) for x in operands]
        + [
            short((HALVES, rows, part, block), half),
            short((HALVES, rows, part, block), half),
            short((POINTS, part, 2 * block), half),
            short((2 * block, block), half),
            short((HALVES, rows, POINTS, part, LANES), half),
            short((HALVES, cols, rows, POINTS, part, LANES), half),
            short((HALVES, w_out.shape[0] // HALVES, features), half),
            short((POINTS, LANES, features), wide),
            dma((steps,)),
            dma((8,)),
            dma((2 * HALVES,)),
            dma((HALVES, rows)),
            dma((HALVES, rows)),
            dma((HALVES, rows)),
            dma((HALVES, rows)),
            dma((HALVES, 3, rows)),
            dma((HALVES, 3, rows)),
        ],
        compiler_params=pltpu.CompilerParams(
            collective_id=0, has_side_effects=True, vmem_limit_bytes=60 * 1024 * 1024
        ),
    )(*operands)


def fits(mesh):
    return mesh.shape["row"] == POINTS and mesh.shape["col"] == 4


def choose(mesh, *arrays):
    tokens, _, w_in, _ = arrays
    group_local = w_in.shape[1] == GROUP
    tiles = tokens.shape[0] == POINTS * LANES
    return fused(*arrays) if fits(mesh) and group_local and tiles else local(*arrays)


def solution(mesh):
    placed = (P("row", None), P(), P(None, "col"), P(None, "col"))
    return jax.shard_map(
        functools.partial(choose, mesh), mesh=mesh, in_specs=placed, out_specs=P("row", "col"), check_vma=False
    )
```

```python
import functools
import math

import jax
import jax.numpy as jnp
import numpy as np
from jax import lax
from jax.experimental import pallas as pl
from jax.experimental.pallas import tpu as pltpu
from jax.sharding import PartitionSpec as P

GROUP = 256


NORM_EPS = 1e-06


def as_sent(array):

    def short(part):
        return part.astype(jnp.bfloat16) if part.dtype == jnp.float32 else part

    return jax.tree.map(short, array)


def rotation_table(first_index, second_index, spectral_magnitude, factor):
    phase = (first_index * second_index % spectral_magnitude).astype(jnp.float32) * (
        2.0 * math.pi / spectral_magnitude
    )
    return (jnp.cos(phase) * factor, jnp.sin(phase) * factor)


def twiddle(real_input_values, imag_in, freq_index, pos_index, spectral_magnitude):
    cosine, sine = rotation_table(freq_index, pos_index, spectral_magnitude, 1.0)
    return (
        real_input_values * cosine + imag_in * sine,
        imag_in * cosine - real_input_values * sine,
    )


def second_section(stacked, half):
    length_dev = stacked.shape[1]
    stride = min(length_dev, 512)
    positions = lax.broadcasted_iota(jnp.int32, (length_dev, stride), 0)
    real_blocks = []
    imag_blocks = []
    for offset in range(0, length_dev, stride):
        freqs = lax.broadcasted_iota(jnp.int32, (length_dev, stride), 1) + offset
        cosine, sine = rotation_table(positions, freqs, length_dev, 1.0)
        with_cos = jnp.dot(stacked, cosine, precision=lax.Precision.HIGH)
        with_sin = jnp.dot(stacked, sine, precision=lax.Precision.HIGH)
        real_blocks.append(with_cos[:half] + with_sin[half:])
        imag_blocks.append(with_cos[half:] - with_sin[:half])
    return (jnp.concatenate(real_blocks, 1), jnp.concatenate(imag_blocks, 1))


def reorder_positions(arrived):
    channels, row_count, _, block_len = arrived.shape
    return jnp.swapaxes(arrived.reshape(channels, row_count, block_len), 1, 2).reshape(
        channels, row_count * block_len
    )


def local(tokens, norm_gain, w_in, w_out):
    length_dev = tokens.shape[0]
    row_count = lax.axis_size("row")
    col_count = lax.axis_size("col")
    total_len = length_dev * row_count
    widened = tokens.astype(jnp.float32)
    inverse = lax.rsqrt(jnp.mean(widened * widened, axis=1, keepdims=True) + NORM_EPS)
    normed = (widened * inverse * norm_gain[None, :]).astype(jnp.bfloat16)
    projected = lax.dot_general(
        w_in, normed, (((0,), (1,)), ((), ())), preferred_element_type=jnp.float32
    ).astype(jnp.bfloat16)
    channels = projected.shape[0]
    block_len = length_dev // row_count
    small_cos, small_sin = rotation_table(
        lax.broadcasted_iota(jnp.int32, (row_count, row_count), 0),
        lax.broadcasted_iota(jnp.int32, (row_count, row_count), 1),
        row_count,
        1.0 / math.sqrt(total_len),
    )
    per_row = channels // row_count
    arrived = lax.all_to_all(
        projected.reshape(channels, 1, length_dev), "row", split_axis=0, concat_axis=1, tiled=True
    )
    values = arrived.astype(jnp.float32)
    real_one = jnp.einsum("ka,cab->ckb", small_cos, values, precision=lax.Precision.HIGH)
    imag_one = -jnp.einsum("ka,cab->ckb", small_sin, values, precision=lax.Precision.HIGH)
    freq_index = lax.broadcasted_iota(jnp.int32, (row_count, length_dev), 0)
    pos_index = lax.broadcasted_iota(jnp.int32, (row_count, length_dev), 1)
    real_two, imag_two = twiddle(real_one, imag_one, freq_index, pos_index, total_len)
    stacked = jnp.concatenate(
        [
            real_two.reshape(per_row * row_count, length_dev),
            imag_two.reshape(per_row * row_count, length_dev),
        ],
        0,
    )
    real_three, imag_three = second_section(stacked, per_row * row_count)
    shaped = (per_row, row_count, row_count, block_len)
    back_real, back_imag = (
        lax.all_to_all(
            real_three.reshape(shaped).astype(jnp.bfloat16),
            "row",
            split_axis=2,
            concat_axis=0,
            tiled=True,
        ).astype(jnp.float32),
        lax.all_to_all(
            imag_three.reshape(shaped).astype(jnp.bfloat16),
            "row",
            split_axis=2,
            concat_axis=0,
            tiled=True,
        ).astype(jnp.float32),
    )
    spec_real = reorder_positions(back_real)
    spec_imag = reorder_positions(back_imag)
    quarter = length_dev // col_count
    group_cosine_table, group_sine_table = rotation_table(
        lax.broadcasted_iota(jnp.int32, (GROUP, GROUP), 0),
        lax.broadcasted_iota(jnp.int32, (GROUP, GROUP), 1),
        GROUP,
        1.0 / math.sqrt(GROUP),
    )
    real_input_values = lax.all_to_all(
        as_sent(spec_real.reshape(channels, col_count, quarter)),
        "col",
        split_axis=1,
        concat_axis=0,
        tiled=True,
    )
    imag_in = lax.all_to_all(
        as_sent(spec_imag.reshape(channels, col_count, quarter)),
        "col",
        split_axis=1,
        concat_axis=0,
        tiled=True,
    )
    width_all = real_input_values.shape[0]
    item_count = real_input_values.shape[2]
    groups = width_all // GROUP
    real_by_group = real_input_values.reshape(groups, GROUP, item_count)
    imaginary_by_group = imag_in.reshape(groups, GROUP, item_count)
    merged_spectrum = jnp.einsum(
        "hz,azo->aho", group_cosine_table, real_by_group, precision=lax.Precision.HIGH
    )
    merged_spectrum = merged_spectrum + jnp.einsum(
        "hz,azo->aho", group_sine_table, imaginary_by_group, precision=lax.Precision.HIGH
    )
    result = merged_spectrum.reshape(width_all, 1, item_count).astype(jnp.bfloat16)
    spectral = lax.all_to_all(result, "col", split_axis=0, concat_axis=1, tiled=True)
    output = lax.dot_general(
        lax.all_gather(spectral.reshape(channels, length_dev), "col", axis=0, tiled=True),
        w_out,
        (((0,), (0,)), ((), ())),
        preferred_element_type=jnp.float32,
    )
    return output.astype(jnp.bfloat16)


HALVES = 2
POINTS = 8
SPLIT = 1
LANES = 128
MESH = pl.DeviceIdType.MESH


def channel_tables(group, total_len):
    half = group // 2
    index = np.arange(group)
    angle = 2.0 * np.pi * (index[:, None] * index[None, :] % group) / group
    transform = np.concatenate([np.cos(angle[: half + 1]), np.sin(angle[1:half])], 0)
    fold = np.zeros((group, group))
    for k in range(half + 1):
        fold[k, k] = 1.0
        fold[k, -k % group] = 1.0
    for k in range(1, half):
        fold[half + k, group - k] = 1.0
        fold[half + k, k] = -1.0
    return (transform / math.sqrt(group)).astype(jnp.bfloat16), fold.astype(jnp.bfloat16)


def position_tables(block, total_len):
    j = np.arange(block)
    angle = 2.0 * np.pi * (np.arange(POINTS)[:, None] * j[None, :]) / total_len
    twiddles = np.stack([np.cos(angle), np.sin(angle)]).astype(np.float32)
    root = 32
    coarse = 2.0 * np.pi * (np.arange(block // root)[:, None] * root * j[None, :] % block) / block
    fine = 2.0 * np.pi * (np.arange(root)[:, None] * j[None, :] % block) / block
    scale = 1.0 / math.sqrt(total_len)
    coarse = np.stack([np.cos(coarse), np.sin(coarse)]).astype(np.float32)
    fine = np.stack([np.cos(fine) * scale, np.sin(fine) * scale]).astype(np.float32)
    return twiddles, coarse, fine


def eight_points(x):
    a = [x[i] + x[i + 4] for i in range(4)]
    b = [x[i] - x[i + 4] for i in range(4)]
    even, odd = a[0] + a[2], a[1] + a[3]
    root = math.sqrt(0.5)
    minus, plus = root * (b[1] - b[3]), root * (b[1] + b[3])
    one = (b[0] + minus, -b[2] - plus)
    two = (a[0] - a[2], a[3] - a[1])
    three = (b[0] - minus, b[2] - plus)
    return [
        (even + odd, None),
        one,
        two,
        three,
        (even - odd, None),
        (three[0], -three[1]),
        (two[0], -two[1]),
        (one[0], -one[1]),
    ]


def mixer_kernel(
    steps, ahead,
    tokens_hbm, gain_hbm, w_in_hbm, w_out_hbm, forward_hbm, fold_hbm, twiddle_hbm, coarse_hbm, fine_hbm,
    out_ref,
    tokens, gain, w_in, w_out, forward, fold, twiddles, coarse, fine,
    packed, arrived, stage, table, ready, gathered, folded, total,
    token_sem, load_sem, own_sem, send_one, recv_one, send_two, recv_two, send_col, recv_col,
):
    row, col = lax.axis_index("row"), lax.axis_index("col")
    rows = packed.shape[1]
    block, width = packed.shape[3], w_in.shape[1]
    size = block // steps
    part = packed.shape[2]
    flip = lambda index, bit: index + bit - 2 * bit * (index // bit % 2)
    sibling, across = flip(col, 1), flip(col, 2)

    def mate(d):
        index = row
        for bit in (1, 2, 4):
            if d & bit:
                index = flip(index, bit)
        return index

    loads = [
        pltpu.make_async_copy(src, dst, load_sem.at[i])
        for i, (src, dst) in enumerate([
            (w_in_hbm, w_in), (gain_hbm, gain), (forward_hbm, forward), (coarse_hbm, coarse), (fine_hbm, fine),
            (twiddle_hbm, twiddles), (fold_hbm, fold), (w_out_hbm, w_out),
        ])
    ]
    token_loads = [
        pltpu.make_async_copy(
            tokens_hbm.at[pl.ds(p * size, size)], tokens.at[pl.ds(p * size, size)], token_sem.at[p]
        )
        for p in range(steps)
    ]
    for load in loads[:3] + token_loads[:ahead]:
        load.start()

    barrier = pltpu.get_barrier_semaphore()
    peers = [(mate(d), col) for d in range(1, rows)] + [(row, sibling), (row, across)]
    for peer in peers:
        pl.semaphore_signal(barrier, inc=1, device_id=peer, device_id_type=MESH)

    def remote(src, dst, send, recv, device):
        return pltpu.make_async_remote_copy(
            src_ref=src, dst_ref=dst, send_sem=send, recv_sem=recv, device_id=device, device_id_type=MESH
        )

    def first_send(h, d, p=None):
        peer = mate(d)
        where = pl.ds(0, block) if p is None else pl.ds(p * size, size)
        return remote(
            packed.at[h, peer, :, where], arrived.at[h, row, :, where],
            send_one.at[h, d], recv_one.at[h, d], (peer, col),
        )

    order = [4, 5, 6, 7, 2, 3, 1]
    for load in loads[:3]:
        load.wait()
    for p in range(steps):
        token_loads[p].wait()
        if p + ahead < steps:
            token_loads[p + ahead].start()
        elif p + ahead == steps:
            for load in loads[3:]:
                load.start()
        where = slice(p * size, (p + 1) * size)
        wide = tokens[where, :].astype(jnp.float32)
        inverse = lax.rsqrt(jnp.mean(wide * wide, axis=1, keepdims=True) + NORM_EPS)
        normed = (wide * inverse * gain[...]).astype(jnp.bfloat16)
        projected = jnp.dot(normed, w_in[...], preferred_element_type=jnp.float32).astype(jnp.bfloat16)
        kept = lax.dot_general(
            forward[...], projected, (((1,), (1,)), ((), ())), preferred_element_type=jnp.float32
        )
        packed[:, :, :, where] = kept.astype(jnp.bfloat16).reshape(HALVES, rows, part, size)
        if p == 0:
            pl.semaphore_wait(barrier, len(peers))
        for d in order:
            first_send(0, d, p).start()
    for d in order:
        first_send(1, d).start()
    own_one = [
        pltpu.make_async_copy(packed.at[h, row], arrived.at[h, row], own_sem.at[h]) for h in range(HALVES)
    ]
    for copy in own_one:
        copy.start()
    for load in loads[3:]:
        load.wait()

    root = fine.shape[1]

    def table_rows(a, carry):
        cos_a, sin_a = coarse[0, pl.ds(a, 1), :], coarse[1, pl.ds(a, 1), :]
        at = pl.multiple_of(a * root, root)
        table[pl.ds(at, root), :] = (cos_a * fine[0] - sin_a * fine[1]).astype(jnp.bfloat16)
        table[pl.ds(block + at, root), :] = (sin_a * fine[0] + cos_a * fine[1]).astype(jnp.bfloat16)
        return carry

    lax.fori_loop(0, block // root, table_rows, 0)
    cols = w_out.shape[0] // width
    half = width // HALVES
    for c in range(cols):
        rows_out = jnp.dot(
            fold[...], w_out[c * width : (c + 1) * width, :], preferred_element_type=jnp.float32
        ).astype(jnp.bfloat16)
        for h in range(HALVES):
            folded[h, c * half : (c + 1) * half, :] = rows_out[h * half : (h + 1) * half]

    cut = POINTS // SPLIT

    def second_send(g, d):
        h, where = g // SPLIT, pl.ds(g % SPLIT * cut, cut)
        peer = mate(d)
        return remote(
            ready.at[h, peer, where], gathered.at[h, col, row, where],
            send_two.at[g, d], recv_two.at[g, d], (peer, col),
        )

    def keep(g):
        h, where = g // SPLIT, pl.ds(g % SPLIT * cut, cut)
        return pltpu.make_async_copy(
            ready.at[h, row, where], gathered.at[h, col, row, where], own_sem.at[HALVES + g]
        )

    span = 2 * LANES
    count = block // span
    other = (1 - row // (rows // 2)) * (count // 2)
    far, close = order[: rows // 2], order[rows // 2 :]
    for h in range(HALVES):
        own_one[h].wait()
        for d in order:
            first_send(h, d).wait_recv()

        def section(t, carry):
            at = pl.multiple_of(t * LANES, LANES)
            x = [arrived[h, r, :, pl.ds(at, LANES)].astype(jnp.float32) for r in range(rows)]
            points = eight_points(x)
            for k in range(POINTS):
                real, imag = points[k]
                if k > 0:
                    cosine = twiddles[0, k : k + 1, pl.ds(at, LANES)]
                    sine = twiddles[1, k : k + 1, pl.ds(at, LANES)]
                    if imag is None:
                        real, imag = real * cosine, -real * sine
                    else:
                        real, imag = real * cosine + imag * sine, imag * cosine - real * sine
                else:
                    imag = jnp.zeros_like(real)
                if h == 1:
                    place = lax.broadcasted_iota(jnp.int32, real.shape, 0) + row * part
                    plain = place == 0
                    real, imag = jnp.where(plain, real, -imag), jnp.where(plain, imag, real)
                stage[k, :, pl.ds(at, LANES)] = real.astype(jnp.bfloat16)
                stage[k, :, pl.ds(pl.multiple_of(block + at, LANES), LANES)] = imag.astype(jnp.bfloat16)
            return carry

        lax.fori_loop(0, block // LANES, section, 0)
        values = stage[...].reshape(POINTS * part, 2 * block)
        for i in range(count):
            n = lax.rem(other + i, count)
            done = jnp.dot(
                values, table[:, pl.ds(pl.multiple_of(n * span, span), span)], preferred_element_type=jnp.float32
            ).astype(jnp.bfloat16)
            for q in range(2):
                ready[h, 2 * n + q] = done[:, q * LANES : (q + 1) * LANES].reshape(POINTS, part, LANES)
            if i == count // 2 - 1:
                for g in range(h * SPLIT, (h + 1) * SPLIT):
                    for d in far:
                        second_send(g, d).start()
        for g in range(h * SPLIT, (h + 1) * SPLIT):
            for d in close:
                second_send(g, d).start()
            keep(g).start()

    def along(g, way, owner, target, d):
        spot = gathered.at[g // SPLIT, owner, mate(d), pl.ds(g % SPLIT * cut, cut)]
        return remote(spot, spot, send_col.at[g, way, d], recv_col.at[g, way, d], (row, target))

    def to_across(g, d):
        return along(g, 0, col, across, d)

    def to_sibling(g, d):
        return along(g, 1, col, sibling, d)

    def on_to_sibling(g, d):
        return along(g, 2, across, sibling, d)

    near, every = [0] + close[::-1], [0] + close[::-1] + far

    def relay(g, origins):
        for d in origins:
            if d == 0:
                keep(g).wait()
            else:
                second_send(g, d).wait_recv()
            to_across(g, d).start()
            to_sibling(g, d).start()

    def pass_on(g, origins):
        for d in origins:
            to_across(g, d).wait_recv()
            on_to_sibling(g, d).start()

    def collect(g):
        for d in every:
            to_sibling(g, d).wait_recv()
            on_to_sibling(g, d).wait_recv()

    def map_out(h, k):
        spectrum = gathered[h, :, :, k].reshape(cols * rows * part, LANES)
        piece = lax.dot_general(
            spectrum, folded[h], (((0,), (0,)), ((), ())), preferred_element_type=jnp.float32
        )
        total[k] = piece if h == 0 else total[k] + piece

    def map_part(g):
        for k in range(g % SPLIT * cut, (g % SPLIT + 1) * cut):
            map_out(g // SPLIT, k)

    relay(0, every)
    for d in every:
        relay(1, [d])
        pass_on(0, [d])
    collect(0)
    for k, d in enumerate(every):
        map_out(0, k)
        pass_on(1, [d])
    collect(1)
    map_part(1)
    out_ref[...] = jnp.swapaxes(total[...], 0, 1).reshape(out_ref.shape).astype(out_ref.dtype)

    for h in range(HALVES):
        for d in order:
            first_send(h, d).wait_send()
    for g in range(HALVES * SPLIT):
        for d in order:
            second_send(g, d).wait_send()
        for d in every:
            to_across(g, d).wait_send()
            to_sibling(g, d).wait_send()
            on_to_sibling(g, d).wait_send()


def fused(tokens, norm_gain, w_in, w_out):
    rows, cols = lax.axis_size("row"), lax.axis_size("col")
    block, width_in = tokens.shape
    width = w_in.shape[1]
    features = w_out.shape[1]
    part = width // (HALVES * rows)
    steps = 4
    forward, fold = channel_tables(width, block * rows)
    twiddles, coarse, fine = position_tables(block, block * rows)
    half, short, wide = jnp.bfloat16, pltpu.VMEM, jnp.float32
    operands = [tokens, norm_gain[None, :], w_in, w_out, forward, fold, twiddles, coarse, fine]
    operands = [jnp.asarray(x) for x in operands]
    dma = pltpu.SemaphoreType.DMA
    return pl.pallas_call(
        functools.partial(mixer_kernel, steps, 2),
        out_shape=jax.ShapeDtypeStruct((block, features), half),
        in_specs=[pl.BlockSpec(memory_space=pl.ANY)] * len(operands),
        out_specs=pl.BlockSpec(memory_space=pltpu.VMEM),
        scratch_shapes=[short(x.shape, x.dtype) for x in operands]
        + [
            short((HALVES, rows, part, block), half),
            short((HALVES, rows, part, block), half),
            short((POINTS, part, 2 * block), half),
            short((2 * block, block), half),
            short((HALVES, rows, POINTS, part, LANES), half),
            short((HALVES, cols, rows, POINTS, part, LANES), half),
            short((HALVES, w_out.shape[0] // HALVES, features), half),
            short((POINTS, LANES, features), wide),
            dma((steps,)),
            dma((8,)),
            dma((HALVES + HALVES * SPLIT,)),
            dma((HALVES, rows)),
            dma((HALVES, rows)),
            dma((HALVES * SPLIT, rows)),
            dma((HALVES * SPLIT, rows)),
            dma((HALVES * SPLIT, 3, rows)),
            dma((HALVES * SPLIT, 3, rows)),
        ],
        compiler_params=pltpu.CompilerParams(
            collective_id=0, has_side_effects=True, vmem_limit_bytes=60 * 1024 * 1024
        ),
    )(*operands)


def fits(mesh):
    return mesh.shape["row"] == POINTS and mesh.shape["col"] == 4


def choose(mesh, *arrays):
    tokens, _, w_in, _ = arrays
    group_local = w_in.shape[1] == GROUP
    tiles = tokens.shape[0] == POINTS * LANES
    return fused(*arrays) if fits(mesh) and group_local and tiles else local(*arrays)


def solution(mesh):
    placed = (P("row", None), P(), P(None, "col"), P(None, "col"))
    return jax.shard_map(
        functools.partial(choose, mesh), mesh=mesh, in_specs=placed, out_specs=P("row", "col"), check_vma=False
    )
```
